32 devices in a mesh: row: 8 (over z, y), col: 4 (over x, core).
Axes of the slice: x: 2, y: 2, z: 4, core: 2. Of those that a mesh axis runs over, the one named last changes fastest.
Arguments:
- tokens: bfloat16 [2, 16384, 1024], P(None, 'row'), may hold values from -6 to 6
- norm_gain: float32 [1024], replicated, may hold values from 0.1 to 1.9
- w_fourier_in: bfloat16 [1024, 512], P(None, 'col'), may hold values from -0.1875 to 0.1875
- w_gate: bfloat16 [1024, 1024], replicated, may hold values from -0.1875 to 0.1875
- w_spectrum: bfloat16 [512, 1024], replicated, may hold values from -0.25 to 0.25
- w_output: bfloat16 [1024, 1024], P(None, 'col'), may hold values from -0.375 to 0.375
Outputs:
- block_output: bfloat16 [2, 16384, 1024], P(None, 'row', 'col')
The draws below stay inside these ranges and needn't reach their ends.
All inputs are finite; a program needn't handle non-finite values.
Results may differ from the reference program's by a relative error of at most 0.015.
Values may be sent and summed in bfloat16 or wider, within the bound.
A program may use at most 320 MiB of HBM per device.

```python
import jax
import jax.numpy as jnp
from jax import lax

D = 1024
GROUPS = 8
GROUP_WIDTH = 64
FOURIER_WIDTH = 512
SEQS = 2
SEQ = 16384


def block_scale(stream_key, dims, cuts, low, largest):
    gain, own = 1.0, jax.random.fold_in(stream_key, 6)
    for axis_at, parts in cuts:
        steps = jnp.exp(jax.random.uniform(jax.random.fold_in(own, axis_at), (parts,), jnp.float32, low / len(cuts), largest / len(cuts)))
        gain = gain * jnp.repeat(steps, dims[axis_at] // parts).reshape([-1 if axis == axis_at else 1 for axis in range(len(dims))])
    return gain


def normal_values(own_key, dims, spread, bound, split=(), held_as=jnp.bfloat16):
    values = jax.random.normal(own_key, dims, jnp.float32) * spread
    if len(split) > 0:
        values = block_scale(own_key, dims, split, -0.22, 0.18) * values
    return jnp.clip(values, min=-bound, max=bound).astype(held_as)


def setup_inputs(seed: int = 0) -> dict:
    key_list = jax.random.split(jax.random.key(seed), 7)
    return {
        "tokens": normal_values(key_list[0], (SEQS, SEQ, D), 1.0, 6.0, ((1, 8),)),
        "norm_gain": jnp.clip(1.0 + 0.18 * jax.random.normal(key_list[1], (D,), jnp.float32), 0.1, 1.9),
        "w_fourier_in": normal_values(key_list[2], (D, FOURIER_WIDTH), D ** -0.5, 0.1875, ((1, 4),)),
        "w_gate": normal_values(key_list[3], (D, D), D ** -0.5, 0.1875),
        "w_spectrum": normal_values(key_list[4], (FOURIER_WIDTH, D), FOURIER_WIDTH ** -0.5, 0.25),
        "w_output": normal_values(key_list[5], (D, D), (D // 4) ** -0.5, 0.375, ((1, 4),)),
    }


norm_eps = 1e-6


def reference(tokens, norm_gain, w_fourier_in, w_gate, w_spectrum, w_output):
    widened = tokens.astype(jnp.float32)
    inverse = lax.rsqrt(jnp.mean(widened * widened, axis=-1, keepdims=True) + norm_eps)
    normed = (widened * inverse * norm_gain).astype(jnp.bfloat16).reshape(SEQS * SEQ, D)
    fourier_in = jnp.dot(normed, w_fourier_in, preferred_element_type=jnp.float32).astype(jnp.bfloat16)
    grouped = fourier_in.astype(jnp.float32).reshape(SEQS, SEQ, GROUPS, GROUP_WIDTH)
    spectrum = jnp.real(jnp.fft.fft2(grouped, axes=(1, 3), norm="ortho")).astype(jnp.bfloat16)
    spectrum = spectrum.reshape(SEQS * SEQ, FOURIER_WIDTH)
    mixed_pre = jnp.dot(spectrum, w_spectrum, preferred_element_type=jnp.float32).astype(jnp.bfloat16)
    gate_pre = jnp.dot(normed, w_gate, preferred_element_type=jnp.float32)
    mixed = (jax.nn.sigmoid(gate_pre) * mixed_pre.astype(jnp.float32)).astype(jnp.bfloat16)
    block_output = jnp.dot(mixed, w_output, preferred_element_type=jnp.float32).astype(jnp.bfloat16)
    return block_output.reshape(SEQS, SEQ, D)
```

```python
import functools

import jax
import jax.numpy as jnp
import numpy as np
from jax import lax
from jax.experimental import pallas as pl
from jax.experimental.pallas import tpu as pltpu
from jax.sharding import PartitionSpec as P

GROUP_WIDTH = 64
FIRST_LEN = 256


norm_eps = 1e-06


def shortened(value):
    return jax.tree.map(lambda a: a.astype(jnp.bfloat16) if a.dtype == jnp.float32 else a, value)


def over_all(value, axis, dim, absorb, carry):
    whole = jax.tree.map(lambda part: lax.all_gather(part, axis, axis=dim, tiled=True), value)
    return absorb(carry, whole, jnp.int32(0))


def dft_tables(length_in, length_out, period):
    left_index = lax.broadcasted_iota(jnp.int32, (length_in, length_out), 0)
    right_index = lax.broadcasted_iota(jnp.int32, (length_in, length_out), 1)
    angles = (left_index * right_index % period).astype(jnp.float32) * (2.0 * jnp.pi / period)
    return (jnp.cos(angles), jnp.sin(angles))


def transform_first(cube, table):
    return jnp.einsum("cpq,pk->ckq", cube, table, precision=lax.Precision.HIGHEST)


def transform_second(cube, table):
    return jnp.einsum("ckq,qj->cjk", cube, table, precision=lax.Precision.HIGHEST)


def positional(real_part, imag_part):
    rows_count, seq_total = real_part.shape
    second_len = seq_total // FIRST_LEN
    cos_first, sin_first = dft_tables(FIRST_LEN, FIRST_LEN, FIRST_LEN)
    cos_twist, sin_twist = dft_tables(FIRST_LEN, second_len, seq_total)
    cos_second, sin_second = dft_tables(second_len, second_len, second_len)
    real_cube = real_part.reshape(rows_count, FIRST_LEN, second_len)
    imag_cube = imag_part.reshape(rows_count, FIRST_LEN, second_len)
    section_real = transform_first(real_cube, cos_first) + transform_first(imag_cube, sin_first)
    section_imag = transform_first(imag_cube, cos_first) - transform_first(real_cube, sin_first)
    twist_real = section_real * cos_twist + section_imag * sin_twist
    twist_imag = section_imag * cos_twist - section_real * sin_twist
    summed = transform_second(twist_real, cos_second) + transform_second(twist_imag, sin_second)
    norm_scale = 1.0 / jnp.sqrt(jnp.float32(seq_total * GROUP_WIDTH))
    return (summed.reshape(rows_count, seq_total) * norm_scale).astype(jnp.bfloat16)


def on_device(tokens, norm_gain, w_fourier_in, w_gate, w_spectrum, w_output):
    batches, seq_local, features = tokens.shape
    tokens_count = batches * seq_local
    widened = tokens.astype(jnp.float32)
    inverse = lax.rsqrt(jnp.mean(widened * widened, axis=-1, keepdims=True) + norm_eps)
    normed = (widened * inverse * norm_gain).astype(jnp.bfloat16).reshape(tokens_count, features)
    fourier_in = jnp.dot(normed, w_fourier_in, preferred_element_type=jnp.float32).astype(
        jnp.bfloat16
    )
    local_groups = w_fourier_in.shape[1] // GROUP_WIDTH
    grouped = fourier_in.astype(jnp.float32).reshape(batches, seq_local, local_groups, GROUP_WIDTH)
    cos_group, sin_group = dft_tables(GROUP_WIDTH, GROUP_WIDTH, GROUP_WIDTH)
    real_part = jnp.einsum(
        "btgn,nm->bgmt", grouped, cos_group, precision=lax.Precision.HIGHEST
    ).reshape(-1, seq_local)
    imag_part = -jnp.einsum(
        "btgn,nm->bgmt", grouped, sin_group, precision=lax.Precision.HIGHEST
    ).reshape(-1, seq_local)
    real_part = lax.all_to_all(
        shortened(real_part), "row", split_axis=0, concat_axis=1, tiled=True
    ).astype(real_part.dtype)
    imag_part = lax.all_to_all(
        shortened(imag_part), "row", split_axis=0, concat_axis=1, tiled=True
    ).astype(imag_part.dtype)
    spectrum = positional(real_part, imag_part)
    spectrum = lax.all_to_all(spectrum, "row", split_axis=1, concat_axis=0, tiled=True)
    spectrum = spectrum.reshape(batches, local_groups * GROUP_WIDTH, seq_local)
    spectrum = jnp.transpose(spectrum, (0, 2, 1)).reshape(tokens_count, local_groups * GROUP_WIDTH)

    def add_spectrum(running, portion, beginning):
        weight_rows = lax.dynamic_slice_in_dim(w_spectrum, beginning, portion.shape[1], 0)
        return running + jnp.dot(portion, weight_rows, preferred_element_type=jnp.float32)

    mixed_pre = over_all(
        spectrum, "col", 1, add_spectrum, jnp.zeros((tokens_count, features), jnp.float32)
    ).astype(jnp.bfloat16)
    gate_pre = jnp.dot(normed, w_gate, preferred_element_type=jnp.float32)
    mixed = (jax.nn.sigmoid(gate_pre) * mixed_pre.astype(jnp.float32)).astype(jnp.bfloat16)
    result = jnp.dot(mixed, w_output, preferred_element_type=jnp.float32)
    return result.astype(jnp.bfloat16).reshape(batches, seq_local, -1)


MESH = pl.DeviceIdType.MESH
HALF = GROUP_WIDTH // 2


def channel_tables():
    n = np.arange(GROUP_WIDTH)
    fold = np.zeros((GROUP_WIDTH, GROUP_WIDTH))
    unfold = np.zeros((GROUP_WIDTH, GROUP_WIDTH))
    for d in range(GROUP_WIDTH):
        if d <= HALF:
            fold[:, d] = np.cos(2 * np.pi * (n * d % GROUP_WIDTH) / GROUP_WIDTH)
            unfold[d, d] = 1.0
            unfold[d, (GROUP_WIDTH - d) % GROUP_WIDTH] = 1.0
        else:
            m = d - HALF
            fold[:, d] = np.sin(2 * np.pi * (n * m % GROUP_WIDTH) / GROUP_WIDTH)
            unfold[d, m] = -1.0
            unfold[d, GROUP_WIDTH - m] = 1.0
    return fold, unfold


def position_tables(n):
    a = np.arange(n)
    ang = 2 * np.pi * (np.outer(a, a) % n) / n
    first = np.concatenate([np.cos(ang), np.sin(ang)], 0)
    second = np.concatenate([np.cos(ang), np.sin(ang)], 1)
    phi = 2 * np.pi * np.outer(a, a) / (n * n)
    scale = 1.0 / np.sqrt(n * n * GROUP_WIDTH)
    c, s = np.cos(phi) * scale, np.sin(phi) * scale
    twist = np.stack([np.stack([c, s]), np.stack([s, -c])])
    return first, second, twist


def mixer_kernel(
    rows, cols, tok, gain, wp, wg, ws, wo, f1, f2, tw, out,
    tokv, wgv, gate, inv, ysc, osc, s1, x1, s2, spec,
    tsem, wsem, s1s, s1r, s2s, spr, fws,
):
    batches, seq_local, features = tok.shape
    cpd, steps, n = x1.shape[2:]
    me = lax.axis_index("row")
    col = lax.axis_index("col")
    sib = col + 1 - 2 * lax.rem(col, 2)
    chips = cols // 2
    chunk = 4 * n
    chunks = seq_local // chunk

    def peer(i):
        return lax.rem(me + i, rows)

    def xpeer(j):
        return lax.rem(col + 2 * j, cols)

    loads = {}
    for b in range(batches):
        for j in range(chunks):
            part = pl.ds(j * chunk, chunk)
            loads[b, j] = pltpu.make_async_copy(
                tok.at[b, part], tokv.at[b, part], tsem.at[b, j]
            )
            loads[b, j].start()
    wload = pltpu.make_async_copy(wg, wgv, wsem)
    wload.start()

    barrier = pltpu.get_barrier_semaphore()
    for i in range(1, rows):
        pl.semaphore_signal(barrier, inc=1, device_id={"row": peer(i)}, device_id_type=MESH)
    for j in range(1, chips):
        pl.semaphore_signal(barrier, inc=1, device_id={"col": xpeer(j)}, device_id_type=MESH)
    pl.semaphore_signal(barrier, inc=1, device_id={"col": sib}, device_id_type=MESH)

    def project(b):
        for j in range(chunks):
            loads[b, j].wait()
            t = tokv[b, j * chunk:(j + 1) * chunk, :]
            w = t.astype(jnp.float32)
            scale = lax.rsqrt(jnp.mean(w * w, axis=-1, keepdims=True) + norm_eps)
            inv[b, j * chunk:(j + 1) * chunk, :] = scale
            y = jnp.dot(t, wp[...], preferred_element_type=jnp.float32) * scale
            for k in range(4):
                ysc[:, 4 * j + k, :] = y[k * n:(k + 1) * n, :].T
        s1[b] = ysc[...].astype(jnp.bfloat16)

    def first_copy(b, i, src):
        to = peer(i)
        return pltpu.make_async_remote_copy(
            src_ref=s1.at[b, pl.ds(to * cpd, cpd)],
            dst_ref=x1.at[b, src],
            send_sem=s1s.at[b, i],
            recv_sem=s1r.at[b, src],
            device_id={"row": to},
            device_id_type=MESH,
        )

    def send_first(b):
        for i in ORDER(rows):
            first_copy(b, i, me).start()
        x1[b, me] = s1[b, pl.ds(me * cpd, cpd)]

    def wait_first(b):
        for i in range(1, rows):
            first_copy(b, i, peer(i)).wait_recv()

    def gates(b, j):
        part = slice(j * chunk, (j + 1) * chunk)
        g = jnp.dot(tokv[b, part, :], wgv[...], preferred_element_type=jnp.float32)
        half = 0.5 * inv[b, part, :]
        gate[b, part, :] = (0.5 * jnp.tanh(g * half) + 0.5).astype(jnp.bfloat16)

    def transform(b):
        for c in range(cpd):
            kind = (lax.rem(me * cpd + c, GROUP_WIDTH) > HALF).astype(jnp.int32)
            x = x1[b, :, c].reshape(n, n)
            g = jnp.dot(f1[...], x, preferred_element_type=jnp.float32)
            ca, sa = tw[kind, 0], tw[kind, 1]
            u = g[:n] * ca - g[n:] * sa
            v = -(g[:n] * sa + g[n:] * ca)
            t = jnp.concatenate([u.astype(jnp.bfloat16), v.astype(jnp.bfloat16)], axis=1)
            o = lax.dot_general(
                f2[...], t, (((1,), (1,)), ((), ())), preferred_element_type=jnp.float32
            )
            osc[:, c, :] = o
        s2[b] = osc[...].astype(jnp.bfloat16)

    def second_copy(b, i, src):
        to = peer(i)
        return pltpu.make_async_remote_copy(
            src_ref=s2.at[b, pl.ds(to * steps, steps)],
            dst_ref=spec.at[col, b, src],
            send_sem=s2s.at[b, i],
            recv_sem=spr.at[col, b, src],
            device_id={"row": to},
            device_id_type=MESH,
        )

    def send_second(b):
        for i in ORDER(rows):
            second_copy(b, i, me).start()
        spec[col, b, me] = s2[b, pl.ds(me * steps, steps)]

    def share(b, src, owner, slot, to):
        return pltpu.make_async_remote_copy(
            src_ref=spec.at[owner, b, src],
            dst_ref=spec.at[owner, b, src],
            send_sem=fws.at[slot, b, src],
            recv_sem=spr.at[owner, b, src],
            device_id={"col": to},
            device_id_type=MESH,
        )

    def relay_own(b, i):
        src = peer(i)
        if i > 0:
            second_copy(b, i, src).wait_recv()
        for j in range(1, chips):
            share(b, src, col, j - 1, xpeer(j)).start()
        share(b, src, col, chips - 1, sib).start()

    def relay_far(b, i):
        src = peer(i)
        for j in range(1, chips):
            share(b, src, xpeer(j), chips - 1 + j, sib).wait_recv()
            share(b, src, xpeer(j), chips - 1 + j, sib).start()

    def relay_order():
        return [0] + list(RECV(rows))

    def relay(b, i):
        order = relay_order()
        relay_own(b, order[i])
        if i > 1:
            relay_far(b, order[i - 2])

    def relay_tail(b):
        order = relay_order()
        for i in order[-2:]:
            relay_far(b, i)
        for i in order:
            src = peer(i)
            share(b, src, sib, 0, sib).wait_recv()
            for j in range(1, chips):
                share(b, src, lax.rem(sib + 2 * j, cols), 0, sib).wait_recv()

    def finish(b, j):
        part = slice(j * chunk, (j + 1) * chunk)
        pieces = []
        for k in range(4):
            piece = spec[:, b, :, 4 * j + k].reshape(cols * rows * cpd, n)
            pieces.append(piece.T)
        lhs = jnp.concatenate(pieces, axis=0)
        pre = jnp.dot(lhs, ws[...], preferred_element_type=jnp.float32)
        mixed = (gate[b, part, :].astype(jnp.float32) * pre).astype(jnp.bfloat16)
        out[b, part, :] = jnp.dot(
            mixed, wo[...], preferred_element_type=jnp.float32
        ).astype(jnp.bfloat16)

    project(0)
    pl.semaphore_wait(barrier, rows - 1 + chips)
    send_first(0)
    for b in range(1, batches):
        project(b)
        send_first(b)
    wload.wait()
    wgv[...] = (wgv[...].astype(jnp.float32) * gain[...]).astype(jnp.bfloat16)
    for j in range(chunks):
        gates(0, j)
    for b in range(batches):
        wait_first(b)
        transform(b)
        send_second(b)
        if b + 1 < batches:
            for j in range(chunks):
                gates(b + 1, j)
    for i in range(rows):
        relay(0, i)
    relay_tail(0)
    for b in range(batches):
        for j in range(chunks):
            finish(b, j)
            if b + 1 < batches:
                for i in range(j * rows // chunks, (j + 1) * rows // chunks):
                    relay(b + 1, i)
        if b + 1 < batches:
            relay_tail(b + 1)
    for b in range(batches):
        for i in range(1, rows):
            first_copy(b, i, me).wait_send()
            second_copy(b, i, me).wait_send()
        for i in range(rows):
            for slot in range(2 * chips - 1):
                share(b, peer(i), col, slot, sib).wait_send()


def ORDER(rows):
    return range(1, rows)


def RECV(rows):
    return range(rows - 1, 0, -1)


def fused(rows, cols, tokens, norm_gain, w_fourier_in, w_gate, w_spectrum, w_output):
    batches, seq_local, features = tokens.shape
    n = int(round((seq_local * rows) ** 0.5))
    channels = w_fourier_in.shape[1]
    cpd = channels // rows
    steps = seq_local // n
    fold, unfold = channel_tables()
    first, second, twist = position_tables(n)
    local_groups = channels // GROUP_WIDTH
    gained = w_fourier_in.astype(jnp.float32) * norm_gain[:, None]
    wp = jnp.dot(
        gained,
        jnp.asarray(np.kron(np.eye(local_groups), fold), jnp.float32),
        precision=lax.Precision.HIGHEST,
    ).astype(jnp.bfloat16)
    ws = jnp.einsum(
        "dm,gmj->gdj",
        jnp.asarray(unfold, jnp.bfloat16),
        w_spectrum.reshape(-1, GROUP_WIDTH, features),
        preferred_element_type=jnp.float32,
    ).astype(jnp.bfloat16).reshape(-1, features)
    vmem = pl.BlockSpec(memory_space=pltpu.VMEM)
    hbm = pl.BlockSpec(memory_space=pl.ANY)
    chunks = seq_local // (4 * n)
    dma = pltpu.SemaphoreType.DMA
    return pl.pallas_call(
        functools.partial(mixer_kernel, rows, cols),
        out_shape=jax.ShapeDtypeStruct((batches, seq_local, w_output.shape[1]), jnp.bfloat16),
        in_specs=[hbm, vmem, vmem, hbm, vmem, vmem, vmem, vmem, vmem],
        out_specs=vmem,
        scratch_shapes=[
            pltpu.VMEM(tokens.shape, jnp.bfloat16),
            pltpu.VMEM((features, features), jnp.bfloat16),
            pltpu.VMEM((batches, seq_local, features), jnp.bfloat16),
            pltpu.VMEM((batches, seq_local, 1), jnp.float32),
            pltpu.VMEM((channels, steps, n), jnp.float32),
            pltpu.VMEM((n, cpd, n), jnp.float32),
            pltpu.VMEM((batches, channels, steps, n), jnp.bfloat16),
            pltpu.VMEM((batches, rows, cpd, steps, n), jnp.bfloat16),
            pltpu.VMEM((batches, n, cpd, n), jnp.bfloat16),
            pltpu.VMEM((cols, batches, rows, steps, cpd, n), jnp.bfloat16),
            dma((batches, chunks)),
            dma(()),
            dma((batches, rows)),
            dma((batches, rows)),
            dma((batches, rows)),
            dma((cols, batches, rows)),
            dma((cols, batches, rows)),
        ],
        compiler_params=pltpu.CompilerParams(
            collective_id=0, has_side_effects=True, vmem_limit_bytes=60 * 1024 * 1024
        ),
    )(
        tokens, norm_gain[:, None], wp, w_gate, ws, w_output,
        jnp.asarray(first, jnp.bfloat16), jnp.asarray(second, jnp.bfloat16),
        jnp.asarray(twist, jnp.float32),
    )


def body(rows, cols, *args):
    tokens, w_fourier_in = args[0], args[2]
    seq_local, channels = tokens.shape[1], w_fourier_in.shape[1]
    n = int(round((seq_local * rows) ** 0.5))
    fits = (
        n * n == seq_local * rows
        and n % 128 == 0
        and channels % (16 * rows) == 0
        and channels % GROUP_WIDTH == 0
        and seq_local % (16 * n) == 0
        and cols % 2 == 0
    )
    if fits:
        return fused(rows, cols, *args)
    return on_device(*args)


def solution(mesh):
    placed = (P(None, "row", None), P(), P(None, "col"), P(), P(), P(None, "col"))
    return jax.shard_map(
        functools.partial(body, mesh.shape["row"], mesh.shape["col"]),
        mesh=mesh, in_specs=placed, out_specs=P(None, "row", "col"), check_vma=False,
    )
```

```python
import functools

import jax
import jax.numpy as jnp
import numpy as np
from jax import lax
from jax.experimental import pallas as pl
from jax.experimental.pallas import tpu as pltpu
from jax.sharding import PartitionSpec as P

GROUP_WIDTH = 64
FIRST_LEN = 256


norm_eps = 1e-06


def shortened(value):
    return jax.tree.map(lambda a: a.astype(jnp.bfloat16) if a.dtype == jnp.float32 else a, value)


def over_all(value, axis, dim, absorb, carry):
    whole = jax.tree.map(lambda part: lax.all_gather(part, axis, axis=dim, tiled=True), value)
    return absorb(carry, whole, jnp.int32(0))


def dft_tables(length_in, length_out, period):
    left_index = lax.broadcasted_iota(jnp.int32, (length_in, length_out), 0)
    right_index = lax.broadcasted_iota(jnp.int32, (length_in, length_out), 1)
    angles = (left_index * right_index % period).astype(jnp.float32) * (2.0 * jnp.pi / period)
    return (jnp.cos(angles), jnp.sin(angles))


def transform_first(cube, table):
    return jnp.einsum("cpq,pk->ckq", cube, table, precision=lax.Precision.HIGHEST)


def transform_second(cube, table):
    return jnp.einsum("ckq,qj->cjk", cube, table, precision=lax.Precision.HIGHEST)


def positional(real_part, imag_part):
    rows_count, seq_total = real_part.shape
    second_len = seq_total // FIRST_LEN
    cos_first, sin_first = dft_tables(FIRST_LEN, FIRST_LEN, FIRST_LEN)
    cos_twist, sin_twist = dft_tables(FIRST_LEN, second_len, seq_total)
    cos_second, sin_second = dft_tables(second_len, second_len, second_len)
    real_cube = real_part.reshape(rows_count, FIRST_LEN, second_len)
    imag_cube = imag_part.reshape(rows_count, FIRST_LEN, second_len)
    section_real = transform_first(real_cube, cos_first) + transform_first(imag_cube, sin_first)
    section_imag = transform_first(imag_cube, cos_first) - transform_first(real_cube, sin_first)
    twist_real = section_real * cos_twist + section_imag * sin_twist
    twist_imag = section_imag * cos_twist - section_real * sin_twist
    summed = transform_second(twist_real, cos_second) + transform_second(twist_imag, sin_second)
    norm_scale = 1.0 / jnp.sqrt(jnp.float32(seq_total * GROUP_WIDTH))
    return (summed.reshape(rows_count, seq_total) * norm_scale).astype(jnp.bfloat16)


def on_device(tokens, norm_gain, w_fourier_in, w_gate, w_spectrum, w_output):
    batches, seq_local, features = tokens.shape
    tokens_count = batches * seq_local
    widened = tokens.astype(jnp.float32)
    inverse = lax.rsqrt(jnp.mean(widened * widened, axis=-1, keepdims=True) + norm_eps)
    normed = (widened * inverse * norm_gain).astype(jnp.bfloat16).reshape(tokens_count, features)
    fourier_in = jnp.dot(normed, w_fourier_in, preferred_element_type=jnp.float32).astype(
        jnp.bfloat16
    )
    local_groups = w_fourier_in.shape[1] // GROUP_WIDTH
    grouped = fourier_in.astype(jnp.float32).reshape(batches, seq_local, local_groups, GROUP_WIDTH)
    cos_group, sin_group = dft_tables(GROUP_WIDTH, GROUP_WIDTH, GROUP_WIDTH)
    real_part = jnp.einsum(
        "btgn,nm->bgmt", grouped, cos_group, precision=lax.Precision.HIGHEST
    ).reshape(-1, seq_local)
    imag_part = -jnp.einsum(
        "btgn,nm->bgmt", grouped, sin_group, precision=lax.Precision.HIGHEST
    ).reshape(-1, seq_local)
    real_part = lax.all_to_all(
        shortened(real_part), "row", split_axis=0, concat_axis=1, tiled=True
    ).astype(real_part.dtype)
    imag_part = lax.all_to_all(
        shortened(imag_part), "row", split_axis=0, concat_axis=1, tiled=True
    ).astype(imag_part.dtype)
    spectrum = positional(real_part, imag_part)
    spectrum = lax.all_to_all(spectrum, "row", split_axis=1, concat_axis=0, tiled=True)
    spectrum = spectrum.reshape(batches, local_groups * GROUP_WIDTH, seq_local)
    spectrum = jnp.transpose(spectrum, (0, 2, 1)).reshape(tokens_count, local_groups * GROUP_WIDTH)

    def add_spectrum(running, portion, beginning):
        weight_rows = lax.dynamic_slice_in_dim(w_spectrum, beginning, portion.shape[1], 0)
        return running + jnp.dot(portion, weight_rows, preferred_element_type=jnp.float32)

    mixed_pre = over_all(
        spectrum, "col", 1, add_spectrum, jnp.zeros((tokens_count, features), jnp.float32)
    ).astype(jnp.bfloat16)
    gate_pre = jnp.dot(normed, w_gate, preferred_element_type=jnp.float32)
    mixed = (jax.nn.sigmoid(gate_pre) * mixed_pre.astype(jnp.float32)).astype(jnp.bfloat16)
    result = jnp.dot(mixed, w_output, preferred_element_type=jnp.float32)
    return result.astype(jnp.bfloat16).reshape(batches, seq_local, -1)


MESH = pl.DeviceIdType.MESH
HALF = GROUP_WIDTH // 2


def channel_tables():
    n = np.arange(GROUP_WIDTH)
    fold = np.zeros((GROUP_WIDTH, GROUP_WIDTH))
    unfold = np.zeros((GROUP_WIDTH, GROUP_WIDTH))
    for d in range(GROUP_WIDTH):
        if d <= HALF:
            fold[:, d] = np.cos(2 * np.pi * (n * d % GROUP_WIDTH) / GROUP_WIDTH)
            unfold[d, d] = 1.0
            unfold[d, (GROUP_WIDTH - d) % GROUP_WIDTH] = 1.0
        else:
            m = d - HALF
            fold[:, d] = np.sin(2 * np.pi * (n * m % GROUP_WIDTH) / GROUP_WIDTH)
            unfold[d, m] = -1.0
            unfold[d, GROUP_WIDTH - m] = 1.0
    return fold, unfold


def position_tables(n):
    a = np.arange(n)
    ang = 2 * np.pi * (np.outer(a, a) % n) / n
    first = np.concatenate([np.cos(ang), np.sin(ang)], 0)
    second = np.concatenate([np.cos(ang), np.sin(ang)], 1)
    phi = 2 * np.pi * np.outer(a, a) / (n * n)
    scale = 1.0 / np.sqrt(n * n * GROUP_WIDTH)
    c, s = np.cos(phi) * scale, np.sin(phi) * scale
    twist = np.stack([np.stack([c, s]), np.stack([s, -c])])
    return first, second, twist


def mixer_kernel(
    rows, cols, tok, gain, wf, wg, wspec, wout, fold, unfold, f1, f2, tw, out,
    tokv, wgv, wsv, ws, wo, wp, gate, inv, ysc, osc, s1, x1, s2, spec,
    tsem, wsem, s1s, s1r, s2s, spr, fws,
):
    batches, seq_local, features = tok.shape
    cpd, steps, n = x1.shape[2:]
    me = lax.axis_index("row")
    col = lax.axis_index("col")
    sib = col + 1 - 2 * lax.rem(col, 2)
    chips = cols // 2
    chunk = 4 * n
    chunks = seq_local // chunk

    def peer(i):
        return lax.rem(me + i, rows)

    def xpeer(j):
        return lax.rem(col + 2 * j, cols)

    loads = {}
    for b in range(batches):
        for j in range(chunks):
            part = pl.ds(j * chunk, chunk)
            loads[b, j] = pltpu.make_async_copy(
                tok.at[b, part], tokv.at[b, part], tsem.at[b, j]
            )
            loads[b, j].start()
    wload = pltpu.make_async_copy(wg, wgv, wsem.at[0])
    wload.start()
    sload = pltpu.make_async_copy(wspec, wsv, wsem.at[1])
    sload.start()
    oload = pltpu.make_async_copy(wout, wo, wsem.at[2])
    oload.start()

    barrier = pltpu.get_barrier_semaphore()
    for i in range(1, rows):
        pl.semaphore_signal(barrier, inc=1, device_id={"row": peer(i)}, device_id_type=MESH)
    for j in range(1, chips):
        pl.semaphore_signal(barrier, inc=1, device_id={"col": xpeer(j)}, device_id_type=MESH)
    pl.semaphore_signal(barrier, inc=1, device_id={"col": sib}, device_id_type=MESH)

    gained = []
    lanes = 128
    for k in range(features // lanes):
        column = jnp.broadcast_to(gain[:, k * lanes:(k + 1) * lanes], (lanes, lanes)).T
        gained.append(column)
        w = wf[k * lanes:(k + 1) * lanes, :].astype(jnp.float32) * column[:, :1]
        wp[k * lanes:(k + 1) * lanes, :] = jnp.dot(
            w, fold[...], precision=lax.Precision.HIGHEST, preferred_element_type=jnp.float32
        ).astype(jnp.bfloat16)

    def project(b):
        for j in range(chunks):
            loads[b, j].wait()
            t = tokv[b, j * chunk:(j + 1) * chunk, :]
            w = t.astype(jnp.float32)
            scale = lax.rsqrt(jnp.mean(w * w, axis=-1, keepdims=True) + norm_eps)
            inv[b, j * chunk:(j + 1) * chunk, :] = scale
            y = jnp.dot(t, wp[...], preferred_element_type=jnp.float32) * scale
            for k in range(4):
                ysc[:, 4 * j + k, :] = y[k * n:(k + 1) * n, :].T
        s1[b] = ysc[...].astype(jnp.bfloat16)

    def first_copy(b, i, src):
        to = peer(i)
        return pltpu.make_async_remote_copy(
            src_ref=s1.at[b, pl.ds(to * cpd, cpd)],
            dst_ref=x1.at[b, src],
            send_sem=s1s.at[b, i],
            recv_sem=s1r.at[b, src],
            device_id={"row": to},
            device_id_type=MESH,
        )

    def send_first(b):
        for i in ORDER(rows):
            first_copy(b, i, me).start()
        x1[b, me] = s1[b, pl.ds(me * cpd, cpd)]

    def wait_first(b):
        for i in range(1, rows):
            first_copy(b, i, peer(i)).wait_recv()

    def gates(b, j):
        part = slice(j * chunk, (j + 1) * chunk)
        g = jnp.dot(tokv[b, part, :], wgv[...], preferred_element_type=jnp.float32)
        half = 0.5 * inv[b, part, :]
        gate[b, part, :] = (0.5 * jnp.tanh(g * half) + 0.5).astype(jnp.bfloat16)

    def transform(b):
        for c in range(cpd):
            kind = (lax.rem(me * cpd + c, GROUP_WIDTH) > HALF).astype(jnp.int32)
            x = x1[b, :, c].reshape(n, n)
            g = jnp.dot(f1[...], x, preferred_element_type=jnp.float32)
            ca, sa = tw[kind, 0], tw[kind, 1]
            u = g[:n] * ca - g[n:] * sa
            v = -(g[:n] * sa + g[n:] * ca)
            t = jnp.concatenate([u.astype(jnp.bfloat16), v.astype(jnp.bfloat16)], axis=1)
            o = lax.dot_general(
                f2[...], t, (((1,), (1,)), ((), ())), preferred_element_type=jnp.float32
            )
            osc[:, c, :] = o
        s2[b] = osc[...].astype(jnp.bfloat16)

    def second_copy(b, i, src):
        to = peer(i)
        return pltpu.make_async_remote_copy(
            src_ref=s2.at[b, pl.ds(to * steps, steps)],
            dst_ref=spec.at[col, b, src],
            send_sem=s2s.at[b, i],
            recv_sem=spr.at[col, b, src],
            device_id={"row": to},
            device_id_type=MESH,
        )

    def send_second(b):
        for i in ORDER(rows):
            second_copy(b, i, me).start()
        spec[col, b, me] = s2[b, pl.ds(me * steps, steps)]

    def share(b, src, owner, slot, to):
        return pltpu.make_async_remote_copy(
            src_ref=spec.at[owner, b, src],
            dst_ref=spec.at[owner, b, src],
            send_sem=fws.at[slot, b, src],
            recv_sem=spr.at[owner, b, src],
            device_id={"col": to},
            device_id_type=MESH,
        )

    def relay_own(b, i):
        src = peer(i)
        if i > 0:
            second_copy(b, i, src).wait_recv()
        for j in range(1, chips):
            share(b, src, col, j - 1, xpeer(j)).start()
        share(b, src, col, chips - 1, sib).start()

    def relay_far(b, i):
        src = peer(i)
        for j in range(1, chips):
            share(b, src, xpeer(j), chips - 1 + j, sib).wait_recv()
            share(b, src, xpeer(j), chips - 1 + j, sib).start()

    def relay_order():
        return [0] + list(RECV(rows))

    def relay(b, i):
        order = relay_order()
        relay_own(b, order[i])
        if i > 1:
            relay_far(b, order[i - 2])

    def relay_tail(b):
        order = relay_order()
        for i in order[-2:]:
            relay_far(b, i)
        for i in order:
            src = peer(i)
            share(b, src, sib, 0, sib).wait_recv()
            for j in range(1, chips):
                share(b, src, lax.rem(sib + 2 * j, cols), 0, sib).wait_recv()

    def finish(b, j):
        part = slice(j * chunk, (j + 1) * chunk)
        pieces = []
        for k in range(4):
            piece = spec[:, b, :, 4 * j + k].reshape(cols * rows * cpd, n)
            pieces.append(piece.T)
        lhs = jnp.concatenate(pieces, axis=0)
        pre = jnp.dot(lhs, ws[...], preferred_element_type=jnp.float32)
        mixed = (gate[b, part, :].astype(jnp.float32) * pre).astype(jnp.bfloat16)
        out[b, part, :] = jnp.dot(
            mixed, wo[...], preferred_element_type=jnp.float32
        ).astype(jnp.bfloat16)

    project(0)
    pl.semaphore_wait(barrier, rows - 1 + chips)
    send_first(0)
    for b in range(1, batches):
        project(b)
        send_first(b)
    wload.wait()
    for k in range(features // lanes):
        part = slice(k * lanes, (k + 1) * lanes)
        scaled = wgv[part, :].astype(jnp.float32) * gained[k][:, :1]
        wgv[part, :] = scaled.astype(jnp.bfloat16)
    for j in range(chunks):
        gates(0, j)
    sload.wait()
    for k in range(wsv.shape[0] // GROUP_WIDTH):
        part = slice(k * GROUP_WIDTH, (k + 1) * GROUP_WIDTH)
        ws[part, :] = jnp.dot(
            unfold[...], wsv[part, :], preferred_element_type=jnp.float32
        ).astype(jnp.bfloat16)
    oload.wait()
    for b in range(batches):
        wait_first(b)
        transform(b)
        send_second(b)
        if b + 1 < batches:
            for j in range(chunks):
                gates(b + 1, j)
    for i in range(rows):
        relay(0, i)
    relay_tail(0)
    for b in range(batches):
        for j in range(chunks):
            finish(b, j)
            if b + 1 < batches:
                for i in range(j * rows // chunks, (j + 1) * rows // chunks):
                    relay(b + 1, i)
        if b + 1 < batches:
            relay_tail(b + 1)
    for b in range(batches):
        for i in range(1, rows):
            first_copy(b, i, me).wait_send()
            second_copy(b, i, me).wait_send()
        for i in range(rows):
            for slot in range(2 * chips - 1):
                share(b, peer(i), col, slot, sib).wait_send()


def ORDER(rows):
    return range(1, rows)


def RECV(rows):
    return range(rows - 1, 0, -1)


def fused(rows, cols, tokens, norm_gain, w_fourier_in, w_gate, w_spectrum, w_output):
    batches, seq_local, features = tokens.shape
    n = int(round((seq_local * rows) ** 0.5))
    channels = w_fourier_in.shape[1]
    cpd = channels // rows
    steps = seq_local // n
    fold, unfold = channel_tables()
    first, second, twist = position_tables(n)
    local_groups = channels // GROUP_WIDTH
    vmem = pl.BlockSpec(memory_space=pltpu.VMEM)
    hbm = pl.BlockSpec(memory_space=pl.ANY)
    chunks = seq_local // (4 * n)
    dma = pltpu.SemaphoreType.DMA
    return pl.pallas_call(
        functools.partial(mixer_kernel, rows, cols),
        out_shape=jax.ShapeDtypeStruct((batches, seq_local, w_output.shape[1]), jnp.bfloat16),
        in_specs=[hbm, vmem, vmem, hbm, hbm, hbm, vmem, vmem, vmem, vmem, vmem],
        out_specs=vmem,
        scratch_shapes=[
            pltpu.VMEM(tokens.shape, jnp.bfloat16),
            pltpu.VMEM((features, features), jnp.bfloat16),
            pltpu.VMEM(w_spectrum.shape, jnp.bfloat16),
            pltpu.VMEM(w_spectrum.shape, jnp.bfloat16),
            pltpu.VMEM(w_output.shape, jnp.bfloat16),
            pltpu.VMEM(w_fourier_in.shape, jnp.bfloat16),
            pltpu.VMEM((batches, seq_local, features), jnp.bfloat16),
            pltpu.VMEM((batches, seq_local, 1), jnp.float32),
            pltpu.VMEM((channels, steps, n), jnp.float32),
            pltpu.VMEM((n, cpd, n), jnp.float32),
            pltpu.VMEM((batches, channels, steps, n), jnp.bfloat16),
            pltpu.VMEM((batches, rows, cpd, steps, n), jnp.bfloat16),
            pltpu.VMEM((batches, n, cpd, n), jnp.bfloat16),
            pltpu.VMEM((cols, batches, rows, steps, cpd, n), jnp.bfloat16),
            dma((batches, chunks)),
            dma((3,)),
            dma((batches, rows)),
            dma((batches, rows)),
            dma((batches, rows)),
            dma((cols, batches, rows)),
            dma((cols, batches, rows)),
        ],
        compiler_params=pltpu.CompilerParams(
            collective_id=0, has_side_effects=True, vmem_limit_bytes=44 * 1024 * 1024
        ),
    )(
        tokens, norm_gain[None, :], w_fourier_in, w_gate, w_spectrum, w_output,
        jnp.asarray(np.kron(np.eye(local_groups), fold), jnp.float32),
        jnp.asarray(unfold, jnp.bfloat16),
        jnp.asarray(first, jnp.bfloat16), jnp.asarray(second, jnp.bfloat16),
        jnp.asarray(twist, jnp.float32),
    )


def body(rows, cols, *args):
    tokens, w_fourier_in = args[0], args[2]
    seq_local, channels = tokens.shape[1], w_fourier_in.shape[1]
    n = int(round((seq_local * rows) ** 0.5))
    fits = (
        n * n == seq_local * rows
        and n % 128 == 0
        and channels % (16 * rows) == 0
        and channels % GROUP_WIDTH == 0
        and seq_local % (16 * n) == 0
        and cols % 2 == 0
    )
    if fits:
        return fused(rows, cols, *args)
    return on_device(*args)


def solution(mesh):
    placed = (P(None, "row", None), P(), P(None, "col"), P(), P(), P(None, "col"))
    return jax.shard_map(
        functools.partial(body, mesh.shape["row"], mesh.shape["col"]),
        mesh=mesh, in_specs=placed, out_specs=P(None, "row", "col"), check_vma=False,
    )
```
